32 devices in a mesh: sp: 8 (over z, y), dp: 4 (over x, core).
Axes of the slice: x: 2, y: 2, z: 4, core: 2. Of those that a mesh axis runs over, the one named last changes fastest.
Arguments:
- u_pre: bfloat16 [4, 8192, 2048], P('dp', 'sp'), may hold values from -6 to 6
- v_pre: bfloat16 [4, 8192, 2048], P('dp', 'sp'), may hold values from -6 to 6
- d_out: bfloat16 [4, 8192, 2048], P('dp', 'sp'), may hold values from -6 to 6
- w_mix: bfloat16 [16, 128, 128], replicated, may hold values from -0.5 to 0.5
- mix_bias: float32 [16, 128], replicated, may hold values from 0.1 to 1.9
- norm_gain: float32 [16, 128], replicated, may hold values from 0.1 to 1.9
- norm_shift: float32 [16, 128], replicated, may hold values from -3 to 3
- w_out: bfloat16 [2048, 2048], P('dp'), may hold values from -0.125 to 0.125
Outputs:
- grad_u: bfloat16 [4, 8192, 2048], P('dp', 'sp')
- grad_v: bfloat16 [4, 8192, 2048], P('dp', 'sp')
- grad_w_out: float32 [2048, 2048], P('dp')
- grad_w_mix: float32 [16, 128, 128], replicated
- grad_mix_bias: float32 [16, 128], replicated
- grad_gain: float32 [16, 128], replicated
- grad_shift: float32 [16, 128], replicated
The draws below stay inside these ranges and needn't reach their ends.
All inputs are finite; a program needn't handle non-finite values.
Results may differ from the reference program's by a relative error of at most 0.012.
Values may be sent and summed in bfloat16 or wider, within the bound.
A program may use at most 192 MiB of HBM per device.

```python
import jax
import jax.numpy as jnp
from jax import lax

D = 2048
GROUPS = 16
CHANS = 128
BLOCK = 128
SGU_W = 2048
SEQLEN = 8192
SEQS = 4


def block_scale(stream_key, extent, shards, least, largest):
    def one(axis_at, blocks):
        heights = jax.random.uniform(jax.random.fold_in(jax.random.fold_in(stream_key, 6), axis_at), (blocks,), jnp.float32, least / len(shards), largest / len(shards))
        return jnp.repeat(jnp.exp(heights), extent[axis_at] // blocks).reshape((-1,) + (1,) * (len(extent) - axis_at - 1))

    factor_of = one(*shards[0])
    for cut in shards[1:]:
        factor_of = factor_of * one(*cut)
    return factor_of


def scatter_about(stream_key, shape, spread, bound, split=(), kind=jnp.bfloat16):
    entries = jax.random.normal(stream_key, shape, jnp.float32) * spread
    if len(split) > 0:
        entries = block_scale(stream_key, shape, split, -0.22, 0.18) * entries
    return jnp.clip(entries, min=-bound, max=bound).astype(kind)


def setup_inputs(seed: int = 0) -> dict:
    arg_keys = jax.random.split(jax.random.key(seed), 9)
    u_pre = scatter_about(arg_keys[0], (SEQS, SEQLEN, SGU_W), 1.0, 6.0, ((0, 4), (1, 8)))
    v_pre = scatter_about(arg_keys[1], (SEQS, SEQLEN, SGU_W), 1.0, 6.0, ((0, 4), (1, 8)))
    d_out = scatter_about(arg_keys[2], (SEQS, SEQLEN, D), 1.0, 6.0, ((0, 4), (1, 8)))
    w_mix = scatter_about(arg_keys[3], (GROUPS, BLOCK, BLOCK), BLOCK ** -0.5, 0.5)
    mix_bias = jnp.clip(1.0 + 0.18 * jax.random.normal(arg_keys[4], (GROUPS, BLOCK), jnp.float32), 0.1, 1.9)
    norm_gain = jnp.clip(1.0 + 0.18 * jax.random.normal(arg_keys[5], (GROUPS, CHANS), jnp.float32), 0.1, 1.9)
    norm_shift = scatter_about(arg_keys[6], (GROUPS, CHANS), 0.5, 3.0, (), jnp.float32)
    w_out = scatter_about(arg_keys[7], (SGU_W, D), SGU_W ** -0.5, 0.125, ((0, 4),))
    return {"u_pre": u_pre, "v_pre": v_pre, "d_out": d_out, "w_mix": w_mix, "mix_bias": mix_bias, "norm_gain": norm_gain, "norm_shift": norm_shift, "w_out": w_out}


EPS = 1e-05

def mechanism(grad_s, u_pre, v_pre, w_mix, mix_bias, gain, shift):
    items, length, width = grad_s.shape
    groups, span = (w_mix.shape[0], w_mix.shape[1])
    chans = width // groups
    shape = (items, length // span, span, groups, chans)
    u_val = u_pre.astype(jnp.float32).reshape(shape)
    v_val = v_pre.astype(jnp.float32).reshape(shape)
    cotan = grad_s.astype(jnp.float32).reshape(shape)
    upper, u_back = jax.vjp(jax.nn.gelu, u_val)
    gated, v_back = jax.vjp(jax.nn.gelu, v_val)
    centre = gated - lax.optimization_barrier(jnp.mean(gated, axis=-1, keepdims=True))
    inverse = lax.rsqrt(lax.optimization_barrier(jnp.mean(centre * centre, axis=-1, keepdims=True)) + EPS)
    scaled = centre * inverse
    normed = (scaled * gain + shift).astype(jnp.bfloat16)
    lower = jnp.tril(jnp.ones((span, span), dtype=bool))
    w_low = jnp.where(lower[None], w_mix, jnp.zeros_like(w_mix))
    mixed = jnp.einsum('gts,insgc->intgc', w_low.astype(jnp.float32), normed.astype(jnp.float32))
    mixed = mixed + jnp.transpose(mix_bias)[:, :, None]
    gated_out = (upper * mixed).astype(jnp.bfloat16)
    d_mixed = cotan * upper
    d_mixed_b = d_mixed.astype(jnp.bfloat16)
    grad_u = u_back(cotan * mixed)[0].astype(jnp.bfloat16).reshape(items, length, width)
    grad_bias = jnp.transpose(lax.optimization_barrier(jnp.sum(d_mixed, axis=(0, 1, 4))))
    grad_w = jnp.einsum('intgc,insgc->gts', d_mixed_b.astype(jnp.float32), normed.astype(jnp.float32))
    grad_w = jnp.where(lower[None], grad_w, jnp.zeros_like(grad_w))
    d_normed = jnp.einsum('gts,intgc->insgc', w_low.astype(jnp.float32), d_mixed_b.astype(jnp.float32))
    grad_gain = lax.optimization_barrier(jnp.sum(d_normed * scaled, axis=(0, 1, 2)))
    grad_shift = lax.optimization_barrier(jnp.sum(d_normed, axis=(0, 1, 2)))
    d_scaled = d_normed * gain
    d_gated = inverse * (d_scaled - lax.optimization_barrier(jnp.mean(d_scaled, axis=-1, keepdims=True)) - scaled * lax.optimization_barrier(jnp.mean(d_scaled * scaled, axis=-1, keepdims=True)))
    grad_v = v_back(d_gated)[0].astype(jnp.bfloat16).reshape(items, length, width)
    return (grad_u, grad_v, gated_out.reshape(items, length, width), grad_w, grad_bias, grad_gain, grad_shift)

def reference(u_pre, v_pre, d_out, w_mix, mix_bias, norm_gain, norm_shift, w_out):
    flat_d = d_out.reshape(-1, D)
    grad_s = jnp.dot(flat_d, jnp.transpose(w_out), preferred_element_type=jnp.float32)
    grad_s = grad_s.astype(jnp.bfloat16).reshape(SEQS, SEQLEN, SGU_W)

    def one_sequence(packed):
        cot, upre, vpre = packed
        return mechanism(cot[None], upre[None], vpre[None], w_mix, mix_bias, norm_gain, norm_shift)
    grad_u, grad_v, gated_out, grad_w, grad_bias, grad_gain, grad_shift = lax.map(one_sequence, (grad_s, u_pre, v_pre))
    grad_u = grad_u.reshape(SEQS, SEQLEN, SGU_W)
    grad_v = grad_v.reshape(SEQS, SEQLEN, SGU_W)
    flat_s = gated_out.reshape(-1, SGU_W)
    grad_w_out = jnp.dot(jnp.transpose(flat_s), flat_d, preferred_element_type=jnp.float32)
    return (grad_u, grad_v, grad_w_out, lax.optimization_barrier(jnp.sum(grad_w, axis=0)), lax.optimization_barrier(jnp.sum(grad_bias, axis=0)), lax.optimization_barrier(jnp.sum(grad_gain, axis=0)), lax.optimization_barrier(jnp.sum(grad_shift, axis=0)))
```

```python
import functools

import jax
import jax.numpy as jnp
from jax import lax
from jax.experimental import pallas as pl
from jax.experimental.pallas import tpu as pltpu
from jax.sharding import PartitionSpec as P

EPS = 1e-05
K0 = 0.7978845608028654
K1 = 0.044715
F32 = jnp.float32
BF16 = jnp.bfloat16


def gelu_parts(a):
    sq = a * a
    t = jnp.tanh(a * (K0 + (K0 * K1) * sq))
    half = 0.5 * (1.0 + t)
    return sq, t, half


def gelu(a):
    _, _, half = gelu_parts(a)
    return a * half


def gelu_both(a):
    sq, t, half = gelu_parts(a)
    slope = half + (0.5 * a) * (1.0 - t * t) * (K0 + (3.0 * K0 * K1) * sq)
    return a * half, slope


def norm_parts(gated):
    centre = gated - jnp.mean(gated, axis=-1, keepdims=True)
    inverse = lax.rsqrt(jnp.mean(centre * centre, axis=-1, keepdims=True) + EPS)
    return centre * inverse, inverse


def mm(a, b, ca, cb):
    return lax.dot_general(a, b, (((ca,), (cb,)), ((), ())), preferred_element_type=F32)


def kernel(
    dims,
    u_ref, v_ref, d_ref, wmix_ref, bias_ref, gain_ref, shift_ref, w_ref,
    gu_ref, gv_ref, dw_ref, sm_ref,
    wfull, part, rcore, rx, rsp, ag, gs, got, wl_ref, wlt_ref, acc, sbuf, srecv,
    wown_s, wown_r, wx_s, wx_r, wsp_s, wsp_r, wfw_s, wfw_r,
    core_s, core_r, xs_s, xs_r, rs_s, rs_r, ag_s, ag_r,
    s1_s, s1_r, s2_s, s2_r,
):
    n_sp, n_dp, gpc, span, chans, width, rows = dims
    pairs = n_dp // 2
    n_dev = n_sp * n_dp
    nb = rows // span
    s = lax.axis_index("sp")
    dpi = lax.axis_index("dp")
    x = dpi // 2
    c = dpi % 2
    other = 1 - c
    mate = {"sp": s, "dp": 2 * x + other}
    part_rows = span // (n_dev // (n_dp * gpc))

    def rc(src, dst, ssem, rsem, dev):
        return pltpu.make_async_remote_copy(
            src_ref=src, dst_ref=dst, send_sem=ssem, recv_sem=rsem,
            device_id=dev, device_id_type=pl.DeviceIdType.MESH,
        )

    def each(lo, hi, fn):
        def body(i, carry):
            fn(i)
            return carry
        lax.fori_loop(lo, hi, body, 0)

    def up(k):
        return (x + k) % pairs

    def down(k):
        return (x + pairs - k) % pairs

    def w_own():
        return rc(w_ref, wfull.at[dpi], wown_s, wown_r, mate)

    def w_x(k):
        return rc(w_ref.at[s], wfull.at[dpi, s], wx_s.at[k], wx_r.at[k], {"sp": s, "dp": 2 * up(k) + c})

    def w_sp(k, o):
        src = 2 * down(k) + c
        return rc(wfull.at[src, s], wfull.at[src, s], wsp_s.at[k, o], wsp_r.at[k, o], {"sp": (s + o) % n_sp, "dp": dpi})

    def w_fw(k):
        src = 2 * down(k) + c
        return rc(wfull.at[src], wfull.at[src], wfw_s.at[k], wfw_r.at[k], mate)

    def gid(xx, cc, q):
        return (2 * xx + cc) * gpc + q

    def t_core(k, q):
        return rc(part.at[gid(up(k), other, q)], rcore.at[k, q], core_s.at[k, q], core_r.at[k, q], mate)

    def t_x(k, q):
        return rc(part.at[gid(up(k), c, q)], rx.at[k, q], xs_s.at[k, q], xs_r.at[k, q], {"sp": s, "dp": 2 * up(k) + c})

    def t_rs(q, o):
        to = (s + o) % n_sp
        return rc(part.at[gid(x, c, q), to], rsp.at[q, o], rs_s.at[q, o], rs_r.at[q, o], {"sp": to, "dp": dpi})

    def t_ag(q, o):
        to = (s + o) % n_sp
        return rc(ag.at[q, s], ag.at[q, s], ag_s.at[q, o], ag_r.at[q, o], {"sp": to, "dp": dpi})

    me = s * n_dp + dpi

    def t_s1(o):
        to = (me + o) % n_dev
        return rc(sbuf.at[to], srecv.at[o], s1_s.at[o], s1_r.at[o], {"sp": to // n_dp, "dp": to % n_dp})

    def t_s2(o):
        to = (me + o) % n_dev
        return rc(sbuf.at[me], srecv.at[n_dev + me], s2_s.at[o], s2_r.at[o], {"sp": to // n_dp, "dp": to % n_dp})

    row = lax.broadcasted_iota(jnp.int32, (span, span), 0)
    col = lax.broadcasted_iota(jnp.int32, (span, span), 1)
    lower = row >= col

    w_own().start()
    for k in range(1, pairs):
        w_x(k).start()
    wfull[dpi] = w_ref[...]

    def lanes(g):
        return pl.ds(pl.multiple_of(g * chans, chans), chans)

    def forward_group(g, half):
        wl = jnp.where(lower, wmix_ref[g], jnp.zeros((), BF16))
        bias = bias_ref[g]
        gain = gain_ref[g]
        shift = shift_ref[g]
        for b in range(nb):
            at = pl.ds(b * span, span)
            scaled, _ = norm_parts(gelu(v_ref[at, lanes(g)].astype(F32)))
            normed = (scaled * gain + shift).astype(BF16)
            mixed = mm(wl, normed, 1, 0) + bias
            out = (gelu(u_ref[at, lanes(g)].astype(F32)) * mixed).astype(BF16)
            got[pl.ds(pl.multiple_of(half * span, span), span), pl.ds(b * span, span)] = out.T

    def core_sum(k, q):
        t_core(k, q).wait_recv()
        g = gid(up(k), c, q)

        def one(j):
            part[g, j] = (part[g, j].astype(F32) + rcore[k, q, j].astype(F32)).astype(BF16)
        each(0, n_sp, one)
        t_x(k, q).start()

    def forward_step(i):
        k = (i // gpc + 1) % pairs
        q = i % gpc
        keep = gid(up(k), c, q)
        give = gid(up(k), other, q)
        each(0, 2, lambda h: forward_group(gid(up(k), (c + h) % 2, q), h))

        def one(j):
            r = mm(got[...], d_ref[:, pl.ds(pl.multiple_of(j * width, width), width)], 1, 0)
            part[keep, j] = r[:span].astype(BF16)
            part[give, j] = r[span:].astype(BF16)
        each(0, n_sp, one)
        t_core(k, q).start()
        last = i - 1

        @pl.when((i > 0) & (last < (pairs - 1) * gpc))
        def _():
            core_sum((last // gpc + 1) % pairs, last % gpc)

    n_far = (pairs - 1) * gpc
    each(0, n_far, forward_step)
    for k in range(1, pairs):
        w_x(k).wait_recv()
        each(1, n_sp, lambda o: w_sp(k, o).start())
    each(n_far, n_far + gpc, forward_step)
    w_own().wait_recv()

    def forward_w():
        for k in range(1, pairs):
            each(1, n_sp, lambda o: w_sp(k, o).wait_recv())
            w_fw(k).start()

    def rs_start(q):
        t_core(0, q).wait_recv()
        for k in range(1, pairs):
            t_x(k, q).wait_recv()
        g = gid(x, c, q)

        def one(j):
            total = part[g, j].astype(F32) + rcore[0, q, j].astype(F32)
            for k in range(1, pairs):
                total = total + rx[k, q, j].astype(F32)
            part[g, j] = total.astype(BF16)
        each(0, n_sp, one)
        each(1, n_sp, lambda o: t_rs(q, o).start())

    def ag_start(q):
        each(1, n_sp, lambda o: t_rs(q, o).wait_recv())
        total = part[gid(x, c, q), s].astype(F32)
        for o in range(1, n_sp):
            total = total + rsp[q, o].astype(F32)
        ag[q, s] = total.astype(BF16)
        each(1, n_sp, lambda o: t_ag(q, o).start())

    sbuf[...] = jnp.zeros_like(sbuf)

    def backward_group(g, half):
        wl = jnp.where(lower, wmix_ref[g], jnp.zeros((), BF16))
        wlt = wl.T
        bias = bias_ref[g]
        gain = gain_ref[g]
        shift = shift_ref[g]
        acc[...] = jnp.zeros_like(acc)
        wl_ref[...] = wl
        wlt_ref[...] = wlt
        hl = pl.ds(pl.multiple_of(half * chans, chans), chans)
        for b in range(nb):
            at = pl.ds(b * span, span)
            gated, v_slope = gelu_both(v_ref[at, lanes(g)].astype(F32))
            scaled, inverse = norm_parts(gated)
            normed = (scaled * gain + shift).astype(BF16)
            mixed = mm(wl_ref[...], normed, 1, 0) + bias
            upper, u_slope = gelu_both(u_ref[at, lanes(g)].astype(F32))
            cot = gs[at, hl].astype(F32)
            dm = cot * upper
            dmb = dm.astype(BF16)
            gu_ref[at, lanes(g)] = (cot * mixed * u_slope).astype(BF16)
            acc[0] += dm
            acc[1] += mm(dmb, normed, 1, 1)
            dn = mm(wlt_ref[...], dmb, 1, 0)
            acc[2] += dn * scaled
            acc[3] += dn
            e = dn * gain
            m1 = jnp.mean(e, axis=-1, keepdims=True)
            m2 = jnp.mean(e * scaled, axis=-1, keepdims=True)
            gv_ref[at, lanes(g)] = (v_slope * (inverse * (e - m1 - scaled * m2))).astype(BF16)
        grad_w = jnp.where(lower, acc[1], 0.0)
        per = span // part_rows
        for p in range(per):
            sbuf[g * per + p, 0:part_rows, :] = grad_w[p * part_rows : (p + 1) * part_rows].astype(BF16)
        g_bias = jnp.sum(acc[0].T, axis=0, keepdims=True)
        g_gain = jnp.sum(acc[2], axis=0, keepdims=True)
        g_shift = jnp.sum(acc[3], axis=0, keepdims=True)
        r16 = lax.broadcasted_iota(jnp.int32, (16, chans), 0)
        extra = jnp.where(r16 == 0, g_bias, jnp.where(r16 == 1, g_gain, jnp.where(r16 == 2, g_shift, 0.0)))
        sbuf[g * per, part_rows : part_rows + 16, :] = extra.astype(BF16)

    per_chunk = gpc // 2
    rs_rows = wfull.shape[2]

    def backward_step(i):
        turn = i // per_chunk
        k = turn // 2
        chunk = 2 * down(k) + (c + turn) % 2
        two = i % per_chunk
        first = 2 * span // rs_rows
        wrows = wfull[chunk, pl.ds(two * first, first)].reshape(2 * span, wfull.shape[3])

        def one(j):
            at = pl.ds(pl.multiple_of(j * 2 * span, 2 * span), 2 * span)
            gs[at, :] = mm(d_ref[at, :], wrows, 1, 1).astype(BF16)
        each(0, rows // (2 * span), one)
        each(0, 2, lambda h: backward_group(chunk * gpc + 2 * two + h, h))

    n_steps = n_dp * per_chunk
    actions = {}

    def put(step, fn):
        actions.setdefault(min(step, n_steps - 1), []).append(fn)

    put(0, forward_w)
    for q in range(gpc):
        put(2 * per_chunk - 2 + (q * n_steps) // (2 * gpc) + q // 2, functools.partial(rs_start, q))
        put(2 * per_chunk - 1 + (q * n_steps) // (2 * gpc) + q // 2, functools.partial(ag_start, q))
    for k in range(1, pairs):
        put(2 * per_chunk * k - 1, lambda k=k: None)

    def whole_step(i):
        turn = i // per_chunk
        for k in range(1, pairs):
            @pl.when(i == (2 * k + 1) * per_chunk)
            def _(k=k):
                w_fw(k).wait_recv()
        backward_step(i)
        for step in sorted(actions):
            @pl.when(i == step)
            def _(step=step):
                for fn in actions[step]:
                    fn()

    core_sum_last = n_far - 1
    del core_sum_last
    each(0, n_steps, whole_step)

    each(1, n_dev, lambda o: t_s1(o).start())
    each(1, n_dev, lambda o: t_s1(o).wait_recv())
    acc_s = sbuf[me].astype(F32)
    acc_s = lax.fori_loop(1, n_dev, lambda o, a: a + srecv[o].astype(F32), acc_s)
    each(1, n_dev, lambda o: t_s1(o).wait_send())
    sbuf[me] = acc_s.astype(BF16)
    srecv[n_dev + me] = acc_s.astype(BF16)
    each(1, n_dev, lambda o: t_s2(o).start())

    for q in range(gpc):
        each(1, n_sp, lambda o: t_ag(q, o).wait_recv())
        for j in range(n_sp):
            dw_ref[q * span : (q + 1) * span, j * width : (j + 1) * width] = ag[q, j]

    each(1, n_dev, lambda o: t_s2(o).wait_recv())
    sm_ref[...] = srecv[n_dev : 2 * n_dev]

    w_own().wait_send()
    for k in range(1, pairs):
        w_x(k).wait_send()
        each(1, n_sp, lambda o: w_sp(k, o).wait_send())
        w_fw(k).wait_send()
        each(0, gpc, lambda q: t_x(k, q).wait_send())
    for k in range(pairs):
        each(0, gpc, lambda q: t_core(k, q).wait_send())
    for q in range(gpc):
        each(1, n_sp, lambda o: t_rs(q, o).wait_send())
        each(1, n_sp, lambda o: t_ag(q, o).wait_send())
    each(1, n_dev, lambda o: t_s2(o).wait_send())


def on_device(n_sp, n_dp, u_pre, v_pre, d_out, w_mix, mix_bias, norm_gain, norm_shift, w_out):
    _, rows, wide = u_pre.shape
    depth = d_out.shape[2]
    groups, span = w_mix.shape[:2]
    chans = wide // groups
    gpc = groups // n_dp
    width = depth // n_sp
    n_dev = n_sp * n_dp
    per = n_dev // groups
    part_rows = span // per
    shard = w_out.shape[0]
    pairs = n_dp // 2
    dims = (n_sp, n_dp, gpc, span, chans, width, rows)
    dma = pltpu.SemaphoreType.DMA
    vm = pltpu.VMEM
    piece = (n_sp, span, width)
    scratch = [
        vm((n_dp, n_sp, shard // n_sp, depth), BF16),
        vm((groups,) + piece, BF16),
        vm((pairs, gpc) + piece, BF16),
        vm((pairs, gpc) + piece, BF16),
        vm((gpc,) + piece, BF16),
        vm((gpc,) + piece, BF16),
        vm((rows, 2 * chans), BF16),
        vm((2 * chans, rows), BF16),
        vm((span, span), BF16),
        vm((span, span), BF16),
        vm((4, span, chans), F32),
        vm((n_dev, part_rows + 16, chans), BF16),
        vm((2 * n_dev, part_rows + 16, chans), BF16),
        dma, dma,
        dma((pairs,)), dma((pairs,)),
        dma((pairs, n_sp)), dma((pairs, n_sp)),
        dma((pairs,)), dma((pairs,)),
        dma((pairs, gpc)), dma((pairs, gpc)),
        dma((pairs, gpc)), dma((pairs, gpc)),
        dma((gpc, n_sp)), dma((gpc, n_sp)),
        dma((gpc, n_sp)), dma((gpc, n_sp)),
        dma((n_dev,)), dma((n_dev,)),
        dma((n_dev,)), dma((n_dev,)),
    ]
    spec = pl.BlockSpec(memory_space=pltpu.VMEM)
    gu, gv, dw, sm = pl.pallas_call(
        functools.partial(kernel, dims),
        out_shape=(
            jax.ShapeDtypeStruct((rows, wide), BF16),
            jax.ShapeDtypeStruct((rows, wide), BF16),
            jax.ShapeDtypeStruct((shard, depth), BF16),
            jax.ShapeDtypeStruct((n_dev, part_rows + 16, chans), BF16),
        ),
        in_specs=[spec] * 8,
        out_specs=(spec,) * 4,
        scratch_shapes=scratch,
        compiler_params=pltpu.CompilerParams(has_side_effects=True, vmem_limit_bytes=67043328),
    )(
        u_pre[0], v_pre[0], d_out[0], w_mix,
        jnp.broadcast_to(mix_bias[:, :, None], (groups, span, chans)),
        norm_gain[:, None, :], norm_shift[:, None, :],
        w_out.reshape(n_sp, shard // n_sp, depth),
    )
    grad_w = sm[:, :part_rows].reshape(groups, span, span).astype(F32)
    extra = sm.reshape(groups, per, part_rows + 16, chans)[:, 0, part_rows:].astype(F32)
    return (gu[None], gv[None], dw.astype(F32), grad_w, extra[:, 0], extra[:, 1], extra[:, 2])


def solution(mesh):
    body = functools.partial(on_device, mesh.shape["sp"], mesh.shape["dp"])
    return jax.shard_map(
        body,
        mesh=mesh,
        in_specs=(
            P("dp", "sp", None),
            P("dp", "sp", None),
            P("dp", "sp", None),
            P(),
            P(),
            P(),
            P(),
            P("dp", None),
        ),
        out_specs=(P("dp", "sp", None), P("dp", "sp", None), P("dp", None), P(), P(), P(), P()),
        check_vma=False,
    )
```

```python
import functools

import jax
import jax.numpy as jnp
from jax import lax
from jax.experimental import pallas as pl
from jax.experimental.pallas import tpu as pltpu
from jax.sharding import PartitionSpec as P

EPS = 1e-05
K0 = 0.7978845608028654
K1 = 0.044715
F32 = jnp.float32
BF16 = jnp.bfloat16


def gelu_parts(a):
    sq = a * a
    t = jnp.tanh(a * (K0 + (K0 * K1) * sq))
    half = 0.5 * (1.0 + t)
    return sq, t, half


def gelu(a):
    _, _, half = gelu_parts(a)
    return a * half


def gelu_both(a):
    sq, t, half = gelu_parts(a)
    slope = half + (0.5 * a) * (1.0 - t * t) * (K0 + (3.0 * K0 * K1) * sq)
    return a * half, slope


def norm_parts(gated):
    centre = gated - jnp.mean(gated, axis=-1, keepdims=True)
    inverse = lax.rsqrt(jnp.mean(centre * centre, axis=-1, keepdims=True) + EPS)
    return centre * inverse, inverse


def mm(a, b, ca, cb):
    return lax.dot_general(a, b, (((ca,), (cb,)), ((), ())), preferred_element_type=F32)


def kernel(
    dims,
    u_ref, v_ref, d_ref, wmix_ref, bias_ref, gain_ref, shift_ref, w_ref,
    gu_ref, gv_ref, dw_ref, sm_ref,
    wfull, part, rcore, rx, ry, rz, ag, gs, got, wl_ref, wlt_ref, acc, sbuf, srecv,
    wown_s, wown_r, wx_s, wx_r, wz_s, wz_r, wy_s, wy_r, wfw_s, wfw_r,
    core_s, core_r, xs_s, xs_r, yr_s, yr_r, zr_s, zr_r, za_s, za_r, ya_s, ya_r,
    s1_s, s1_r, s2_s, s2_r,
):
    n_y, n_z, n_dp, gpc, span, chans, width, rows = dims
    n_sp = n_y * n_z
    pairs = n_dp // 2
    n_dev = n_sp * n_dp
    nb = rows // span
    s = lax.axis_index("sp")
    dpi = lax.axis_index("dp")
    x = dpi // 2
    c = dpi % 2
    y = s % n_y
    z = s // n_y
    zp = z % 2
    other = 1 - c
    mate = {"sp": s, "dp": 2 * x + other}
    part_rows = span // (n_dev // (n_dp * gpc))

    def rc(src, dst, ssem, rsem, dev):
        return pltpu.make_async_remote_copy(
            src_ref=src, dst_ref=dst, send_sem=ssem, recv_sem=rsem,
            device_id=dev, device_id_type=pl.DeviceIdType.MESH,
        )

    def each(lo, hi, fn):
        def body(i, carry):
            fn(i)
            return carry
        lax.fori_loop(lo, hi, body, 0)

    def up(k):
        return (x + k) % pairs

    def down(k):
        return (x + pairs - k) % pairs

    def w_own():
        return rc(w_ref, wfull.at[dpi], wown_s, wown_r, mate)

    def at_y(o):
        return {"sp": z * n_y + (y + o) % n_y, "dp": dpi}

    def at_z(o):
        return {"sp": (z + o) % n_z * n_y + y, "dp": dpi}

    def w_x(k):
        return rc(w_ref.at[y, zp], wfull.at[dpi, y, zp], wx_s.at[k], wx_r.at[k], {"sp": s, "dp": 2 * up(k) + c})

    def w_z(k):
        src = 2 * down(k) + c
        to = {"sp": (z + 1 - 2 * zp) * n_y + y, "dp": dpi}
        return rc(wfull.at[src, y, zp], wfull.at[src, y, zp], wz_s.at[k], wz_r.at[k], to)

    def w_y(k, h, o):
        src = 2 * down(k) + c
        block = wfull.at[src, y, (zp + h) % 2]
        return rc(block, block, wy_s.at[k, (zp + h) % 2, o], wy_r.at[k, (zp + h) % 2, o], at_y(o))

    def w_fw(k):
        src = 2 * down(k) + c
        return rc(wfull.at[src], wfull.at[src], wfw_s.at[k], wfw_r.at[k], mate)

    def gid(xx, cc, q):
        return (2 * xx + cc) * gpc + q

    def t_core(k, q):
        return rc(part.at[gid(up(k), other, q)], rcore.at[k, q], core_s.at[k, q], core_r.at[k, q], mate)

    def t_x(k, q):
        return rc(part.at[gid(up(k), c, q)], rx.at[k, q], xs_s.at[k, q], xs_r.at[k, q], {"sp": s, "dp": 2 * up(k) + c})

    def t_yr(q, o):
        return rc(part.at[gid(x, c, q), (y + o) % n_y], ry.at[q, o], yr_s.at[q, o], yr_r.at[q, o], at_y(o))

    def t_zr(q, o):
        return rc(part.at[gid(x, c, q), y, (z + o) % n_z], rz.at[q, o], zr_s.at[q, o], zr_r.at[q, o], at_z(o))

    def t_za(q, o):
        return rc(ag.at[q, y, z], ag.at[q, y, z], za_s.at[q, o], za_r.at[q, o], at_z(o))

    def t_ya(q, o):
        return rc(ag.at[q, y], ag.at[q, y], ya_s.at[q, o], ya_r.at[q, o], at_y(o))

    me = s * n_dp + dpi

    def t_s1(o):
        to = (me + o) % n_dev
        return rc(sbuf.at[to], srecv.at[o], s1_s.at[o], s1_r.at[o], {"sp": to // n_dp, "dp": to % n_dp})

    def t_s2(o):
        to = (me + o) % n_dev
        return rc(sbuf.at[me], srecv.at[n_dev + me], s2_s.at[o], s2_r.at[o], {"sp": to // n_dp, "dp": to % n_dp})

    row = lax.broadcasted_iota(jnp.int32, (span, span), 0)
    col = lax.broadcasted_iota(jnp.int32, (span, span), 1)
    lower = row >= col

    w_own().start()
    for k in range(1, pairs):
        w_x(k).start()
    wfull[dpi] = w_ref[...]

    def lanes(g):
        return pl.ds(pl.multiple_of(g * chans, chans), chans)

    def forward_group(g, half):
        wl = jnp.where(lower, wmix_ref[g], jnp.zeros((), BF16))
        bias = bias_ref[g]
        gain = gain_ref[g]
        shift = shift_ref[g]
        for b in range(nb):
            at = pl.ds(b * span, span)
            scaled, _ = norm_parts(gelu(v_ref[at, lanes(g)].astype(F32)))
            normed = (scaled * gain + shift).astype(BF16)
            mixed = mm(wl, normed, 1, 0) + bias
            out = (gelu(u_ref[at, lanes(g)].astype(F32)) * mixed).astype(BF16)
            got[pl.ds(pl.multiple_of(half * span, span), span), pl.ds(b * span, span)] = out.T

    def core_sum(k, q):
        t_core(k, q).wait_recv()
        g = gid(up(k), c, q)

        def one(j):
            a, b = j // n_z, j % n_z
            part[g, a, b] = (part[g, a, b].astype(F32) + rcore[k, q, a, b].astype(F32)).astype(BF16)
        each(0, n_sp, one)
        t_x(k, q).start()

    def forward_step(i):
        k = (i // gpc + 1) % pairs
        q = i % gpc
        keep = gid(up(k), c, q)
        give = gid(up(k), other, q)
        each(0, 2, lambda h: forward_group(gid(up(k), (c + h) % 2, q), h))

        def one(j):
            r = mm(got[...], d_ref[:, pl.ds(pl.multiple_of(j * width, width), width)], 1, 0)
            part[keep, j // n_z, j % n_z] = r[:span].astype(BF16)
            part[give, j // n_z, j % n_z] = r[span:].astype(BF16)
        each(0, n_sp, one)
        t_core(k, q).start()
        last = i - 1

        @pl.when((i > 0) & (last < (pairs - 1) * gpc))
        def _():
            core_sum((last // gpc + 1) % pairs, last % gpc)

    n_far = (pairs - 1) * gpc
    each(0, n_far // 2, forward_step)
    for k in range(1, pairs):
        w_x(k).wait_recv()
        w_z(k).start()
        each(1, n_y, lambda o: w_y(k, 0, o).start())
    each(n_far // 2, n_far + 1, forward_step)
    for k in range(1, pairs):
        w_z(k).wait_recv()
        each(1, n_y, lambda o: w_y(k, 1, o).start())
    each(n_far + 1, n_far + gpc, forward_step)
    w_own().wait_recv()

    def forward_w():
        for k in range(1, pairs):
            each(1, n_y, lambda o: w_y(k, 0, o).wait_recv())
            each(1, n_y, lambda o: w_y(k, 1, o).wait_recv())
            w_fw(k).start()

    def yr_start(q):
        t_core(0, q).wait_recv()
        for k in range(1, pairs):
            t_x(k, q).wait_recv()
        g = gid(x, c, q)

        def one(j):
            a, b = j // n_z, j % n_z
            total = part[g, a, b].astype(F32) + rcore[0, q, a, b].astype(F32)
            for k in range(1, pairs):
                total = total + rx[k, q, a, b].astype(F32)
            part[g, a, b] = total.astype(BF16)
        each(0, n_sp, one)
        each(1, n_y, lambda o: t_yr(q, o).start())

    def zr_start(q):
        each(1, n_y, lambda o: t_yr(q, o).wait_recv())
        g = gid(x, c, q)

        def one(b):
            total = part[g, y, b].astype(F32)
            for o in range(1, n_y):
                total = total + ry[q, o, b].astype(F32)
            part[g, y, b] = total.astype(BF16)
        each(0, n_z, one)
        each(1, n_z, lambda o: t_zr(q, o).start())

    def za_start(q):
        each(1, n_z, lambda o: t_zr(q, o).wait_recv())
        total = part[gid(x, c, q), y, z].astype(F32)
        for o in range(1, n_z):
            total = total + rz[q, o].astype(F32)
        ag[q, y, z] = total.astype(BF16)
        each(1, n_z, lambda o: t_za(q, o).start())

    def ya_start(q):
        each(1, n_z, lambda o: t_za(q, o).wait_recv())
        each(1, n_y, lambda o: t_ya(q, o).start())

    sbuf[...] = jnp.zeros_like(sbuf)

    def backward_group(g, half):
        wl = jnp.where(lower, wmix_ref[g], jnp.zeros((), BF16))
        wlt = wl.T
        bias = bias_ref[g]
        gain = gain_ref[g]
        shift = shift_ref[g]
        acc[...] = jnp.zeros_like(acc)
        wl_ref[...] = wl
        wlt_ref[...] = wlt
        hl = pl.ds(pl.multiple_of(half * chans, chans), chans)
        for b in range(nb):
            at = pl.ds(b * span, span)
            gated, v_slope = gelu_both(v_ref[at, lanes(g)].astype(F32))
            scaled, inverse = norm_parts(gated)
            normed = (scaled * gain + shift).astype(BF16)
            mixed = mm(wl_ref[...], normed, 1, 0) + bias
            upper, u_slope = gelu_both(u_ref[at, lanes(g)].astype(F32))
            cot = gs[at, hl].astype(F32)
            dm = cot * upper
            dmb = dm.astype(BF16)
            gu_ref[at, lanes(g)] = (cot * mixed * u_slope).astype(BF16)
            acc[0] += dm
            acc[1] += mm(dmb, normed, 1, 1)
            dn = mm(wlt_ref[...], dmb, 1, 0)
            acc[2] += dn * scaled
            acc[3] += dn
            e = dn * gain
            m1 = jnp.mean(e, axis=-1, keepdims=True)
            m2 = jnp.mean(e * scaled, axis=-1, keepdims=True)
            gv_ref[at, lanes(g)] = (v_slope * (inverse * (e - m1 - scaled * m2))).astype(BF16)
        grad_w = jnp.where(lower, acc[1], 0.0)
        per = span // part_rows
        for p in range(per):
            sbuf[g * per + p, 0:part_rows, :] = grad_w[p * part_rows : (p + 1) * part_rows].astype(BF16)
        g_bias = jnp.sum(acc[0].T, axis=0, keepdims=True)
        g_gain = jnp.sum(acc[2], axis=0, keepdims=True)
        g_shift = jnp.sum(acc[3], axis=0, keepdims=True)
        r16 = lax.broadcasted_iota(jnp.int32, (16, chans), 0)
        extra = jnp.where(r16 == 0, g_bias, jnp.where(r16 == 1, g_gain, jnp.where(r16 == 2, g_shift, 0.0)))
        sbuf[g * per, part_rows : part_rows + 16, :] = extra.astype(BF16)

    per_chunk = gpc // 2
    flat = wfull.reshape(n_dp, wfull.shape[1] * 2 * wfull.shape[3], wfull.shape[4])

    def backward_step(i):
        turn = i // per_chunk
        k = turn // 2
        chunk = 2 * down(k) + (c + turn) % 2
        two = i % per_chunk
        wrows = flat[chunk, pl.ds(pl.multiple_of(two * 2 * span, 2 * span), 2 * span), :]

        def one(j):
            at = pl.ds(pl.multiple_of(j * 2 * span, 2 * span), 2 * span)
            gs[at, :] = mm(d_ref[at, :], wrows, 1, 1).astype(BF16)
        each(0, rows // (2 * span), one)
        each(0, 2, lambda h: backward_group(chunk * gpc + 2 * two + h, h))

    n_steps = n_dp * per_chunk
    actions = {}

    def put(step, fn):
        actions.setdefault(min(step, n_steps - 1), []).append(fn)

    put(min(2, 2 * per_chunk - 2), forward_w)
    when = ((-1, 1, 3, 5), (0, 2, 4, 6), (2, 4, 6, 8), (4, 6, 8, 9))
    late = []
    stages = (yr_start, zr_start, za_start, ya_start)
    plan = [(when[q % 4][n], n, q) for q in range(gpc) for n in range(4)]
    for step, n, q in sorted(plan):
        fn = functools.partial(stages[n], q)
        if step < 0:
            fn()
        elif step < n_steps:
            put(step, fn)
        else:
            late.append(fn)

    def whole_step(i):
        turn = i // per_chunk
        for k in range(1, pairs):
            @pl.when(i == (2 * k + 1) * per_chunk)
            def _(k=k):
                w_fw(k).wait_recv()
        backward_step(i)
        for step in sorted(actions):
            @pl.when(i == step)
            def _(step=step):
                for fn in actions[step]:
                    fn()

    each(0, n_steps, whole_step)

    each(1, n_dev, lambda o: t_s1(o).start())
    for fn in late:
        fn()
    each(1, n_dev, lambda o: t_s1(o).wait_recv())
    acc_s = sbuf[me].astype(F32)
    acc_s = lax.fori_loop(1, n_dev, lambda o, a: a + srecv[o].astype(F32), acc_s)
    each(1, n_dev, lambda o: t_s1(o).wait_send())
    sbuf[me] = acc_s.astype(BF16)
    srecv[n_dev + me] = acc_s.astype(BF16)
    each(1, n_dev, lambda o: t_s2(o).start())

    for q in range(gpc):
        each(1, n_y, lambda o: t_ya(q, o).wait_recv())
        for j in range(n_sp):
            dw_ref[q * span : (q + 1) * span, j * width : (j + 1) * width] = ag[q, j // n_z, j % n_z]

    each(1, n_dev, lambda o: t_s2(o).wait_recv())
    sm_ref[...] = srecv[n_dev : 2 * n_dev]

    w_own().wait_send()
    for k in range(1, pairs):
        w_x(k).wait_send()
        w_z(k).wait_send()
        each(1, n_y, lambda o: w_y(k, 0, o).wait_send())
        each(1, n_y, lambda o: w_y(k, 1, o).wait_send())
        w_fw(k).wait_send()
        each(0, gpc, lambda q: t_x(k, q).wait_send())
    for k in range(pairs):
        each(0, gpc, lambda q: t_core(k, q).wait_send())
    for q in range(gpc):
        each(1, n_y, lambda o: t_yr(q, o).wait_send())
        each(1, n_z, lambda o: t_zr(q, o).wait_send())
        each(1, n_z, lambda o: t_za(q, o).wait_send())
        each(1, n_y, lambda o: t_ya(q, o).wait_send())
    each(1, n_dev, lambda o: t_s2(o).wait_send())


def on_device(n_sp, n_dp, u_pre, v_pre, d_out, w_mix, mix_bias, norm_gain, norm_shift, w_out):
    _, rows, wide = u_pre.shape
    depth = d_out.shape[2]
    groups, span = w_mix.shape[:2]
    chans = wide // groups
    gpc = groups // n_dp
    width = depth // n_sp
    n_dev = n_sp * n_dp
    per = n_dev // groups
    part_rows = span // per
    shard = w_out.shape[0]
    pairs = n_dp // 2
    n_y = 1
    while 4 * n_y * n_y <= n_sp:
        n_y *= 2
    n_z = n_sp // n_y
    dims = (n_y, n_z, n_dp, gpc, span, chans, width, rows)
    dma = pltpu.SemaphoreType.DMA
    vm = pltpu.VMEM
    piece = (n_y, n_z, span, width)
    w_piece = (n_y, 2, shard // (2 * n_y), depth)
    scratch = [
        vm((n_dp,) + w_piece, BF16),
        vm((groups,) + piece, BF16),
        vm((pairs, gpc) + piece, BF16),
        vm((pairs, gpc) + piece, BF16),
        vm((gpc,) + piece, BF16),
        vm((gpc,) + piece[1:2] + piece[2:], BF16),
        vm((gpc,) + piece, BF16),
        vm((rows, 2 * chans), BF16),
        vm((2 * chans, rows), BF16),
        vm((span, span), BF16),
        vm((span, span), BF16),
        vm((4, span, chans), F32),
        vm((n_dev, part_rows + 16, chans), BF16),
        vm((2 * n_dev, part_rows + 16, chans), BF16),
        dma, dma,
        dma((pairs,)), dma((pairs,)),
        dma((pairs,)), dma((pairs,)),
        dma((pairs, 2, n_y)), dma((pairs, 2, n_y)),
        dma((pairs,)), dma((pairs,)),
        dma((pairs, gpc)), dma((pairs, gpc)),
        dma((pairs, gpc)), dma((pairs, gpc)),
        dma((gpc, n_y)), dma((gpc, n_y)),
        dma((gpc, n_z)), dma((gpc, n_z)),
        dma((gpc, n_z)), dma((gpc, n_z)),
        dma((gpc, n_y)), dma((gpc, n_y)),
        dma((n_dev,)), dma((n_dev,)),
        dma((n_dev,)), dma((n_dev,)),
    ]
    spec = pl.BlockSpec(memory_space=pltpu.VMEM)
    gu, gv, dw, sm = pl.pallas_call(
        functools.partial(kernel, dims),
        out_shape=(
            jax.ShapeDtypeStruct((rows, wide), BF16),
            jax.ShapeDtypeStruct((rows, wide), BF16),
            jax.ShapeDtypeStruct((shard, depth), BF16),
            jax.ShapeDtypeStruct((n_dev, part_rows + 16, chans), BF16),
        ),
        in_specs=[spec] * 8,
        out_specs=(spec,) * 4,
        scratch_shapes=scratch,
        compiler_params=pltpu.CompilerParams(has_side_effects=True, vmem_limit_bytes=67043328),
    )(
        u_pre[0], v_pre[0], d_out[0], w_mix,
        jnp.broadcast_to(mix_bias[:, :, None], (groups, span, chans)),
        norm_gain[:, None, :], norm_shift[:, None, :],
        w_out.reshape(w_piece),
    )
    grad_w = sm[:, :part_rows].reshape(groups, span, span).astype(F32)
    extra = sm.reshape(groups, per, part_rows + 16, chans)[:, 0, part_rows:].astype(F32)
    return (gu[None], gv[None], dw.astype(F32), grad_w, extra[:, 0], extra[:, 1], extra[:, 2])


def solution(mesh):
    body = functools.partial(on_device, mesh.shape["sp"], mesh.shape["dp"])
    return jax.shard_map(
        body,
        mesh=mesh,
        in_specs=(
            P("dp", "sp", None),
            P("dp", "sp", None),
            P("dp", "sp", None),
            P(),
            P(),
            P(),
            P(),
            P("dp", None),
        ),
        out_specs=(P("dp", "sp", None), P("dp", "sp", None), P("dp", None), P(), P(), P(), P()),
        check_vma=False,
    )
```

```python
import functools

import jax
import jax.numpy as jnp
from jax import lax
from jax.experimental import pallas as pl
from jax.experimental.pallas import tpu as pltpu
from jax.sharding import PartitionSpec as P

EPS = 1e-05
K0 = 0.7978845608028654
K1 = 0.044715
F32 = jnp.float32
BF16 = jnp.bfloat16


def gelu_parts(a):
    sq = a * a
    t = jnp.tanh(a * (K0 + (K0 * K1) * sq))
    half = 0.5 * (1.0 + t)
    return sq, t, half


def gelu(a):
    _, _, half = gelu_parts(a)
    return a * half


def gelu_both(a):
    sq, t, half = gelu_parts(a)
    slope = half + (0.5 * a) * (1.0 - t * t) * (K0 + (3.0 * K0 * K1) * sq)
    return a * half, slope


def norm_parts(gated):
    centre = gated - jnp.mean(gated, axis=-1, keepdims=True)
    inverse = lax.rsqrt(jnp.mean(centre * centre, axis=-1, keepdims=True) + EPS)
    return centre * inverse, inverse


def mm(a, b, ca, cb):
    return lax.dot_general(a, b, (((ca,), (cb,)), ((), ())), preferred_element_type=F32)


def kernel(
    dims,
    u_hbm, v_hbm, d_hbm, wmix_ref, bias_ref, gain_ref, shift_ref, w_ref,
    gu_hbm, gv_hbm, dw_ref, sm_ref,
    u_ref, v_ref, d_ref, gu_ref, gv_ref, in_s, gu_s, gv_s,
    wfull, part, rcore, rx, ry, rz, ag, gs, got, wl_ref, wlt_ref, acc, sbuf, srecv,
    wown_s, wown_r, wx_s, wx_r, wz_s, wz_r, wy_s, wy_r, wfw_s, wfw_r,
    core_s, core_r, xs_s, xs_r, yr_s, yr_r, zr_s, zr_r, za_s, za_r, ya_s, ya_r,
    s1_s, s1_r, s2_s, s2_r,
):
    n_y, n_z, n_dp, gpc, span, chans, width, rows = dims
    n_sp = n_y * n_z
    pairs = n_dp // 2
    n_dev = n_sp * n_dp
    nb = rows // span
    s = lax.axis_index("sp")
    dpi = lax.axis_index("dp")
    x = dpi // 2
    c = dpi % 2
    y = s % n_y
    z = s // n_y
    zp = z % 2
    other = 1 - c
    mate = {"sp": s, "dp": 2 * x + other}
    part_rows = span // (n_dev // (n_dp * gpc))

    def rc(src, dst, ssem, rsem, dev):
        return pltpu.make_async_remote_copy(
            src_ref=src, dst_ref=dst, send_sem=ssem, recv_sem=rsem,
            device_id=dev, device_id_type=pl.DeviceIdType.MESH,
        )

    def each(lo, hi, fn):
        def body(i, carry):
            fn(i)
            return carry
        lax.fori_loop(lo, hi, body, 0)

    def up(k):
        return (x + k) % pairs

    def down(k):
        return (x + pairs - k) % pairs

    def w_own():
        return rc(w_ref, wfull.at[dpi], wown_s, wown_r, mate)

    def at_y(o):
        return {"sp": z * n_y + (y + o) % n_y, "dp": dpi}

    def at_z(o):
        return {"sp": (z + o) % n_z * n_y + y, "dp": dpi}

    def w_x(k):
        return rc(w_ref.at[y, zp], wfull.at[dpi, y, zp], wx_s.at[k], wx_r.at[k], {"sp": s, "dp": 2 * up(k) + c})

    def w_z(k):
        src = 2 * down(k) + c
        to = {"sp": (z + 1 - 2 * zp) * n_y + y, "dp": dpi}
        return rc(wfull.at[src, y, zp], wfull.at[src, y, zp], wz_s.at[k], wz_r.at[k], to)

    def w_y(k, h, o):
        src = 2 * down(k) + c
        block = wfull.at[src, y, (zp + h) % 2]
        return rc(block, block, wy_s.at[k, (zp + h) % 2, o], wy_r.at[k, (zp + h) % 2, o], at_y(o))

    def w_fw(k):
        src = 2 * down(k) + c
        return rc(wfull.at[src], wfull.at[src], wfw_s.at[k], wfw_r.at[k], mate)

    def gid(xx, cc, q):
        return (2 * xx + cc) * gpc + q

    def t_core(k, q):
        return rc(part.at[gid(up(k), other, q)], rcore.at[k, q], core_s.at[k, q], core_r.at[k, q], mate)

    def t_x(k, q):
        return rc(part.at[gid(up(k), c, q)], rx.at[k, q], xs_s.at[k, q], xs_r.at[k, q], {"sp": s, "dp": 2 * up(k) + c})

    def t_yr(q, o):
        return rc(part.at[gid(x, c, q), (y + o) % n_y], ry.at[q, o], yr_s.at[q, o], yr_r.at[q, o], at_y(o))

    def t_zr(q, o):
        return rc(part.at[gid(x, c, q), y, (z + o) % n_z], rz.at[q, o], zr_s.at[q, o], zr_r.at[q, o], at_z(o))

    def t_za(q, o):
        return rc(ag.at[q, y, z], ag.at[q, y, z], za_s.at[q, o], za_r.at[q, o], at_z(o))

    def t_ya(q, o):
        return rc(ag.at[q, y], ag.at[q, y], ya_s.at[q, o], ya_r.at[q, o], at_y(o))

    me = s * n_dp + dpi

    def t_s1(o):
        to = (me + o) % n_dev
        return rc(sbuf.at[to], srecv.at[o], s1_s.at[o], s1_r.at[o], {"sp": to // n_dp, "dp": to % n_dp})

    def t_s2(o):
        to = (me + o) % n_dev
        return rc(sbuf.at[me], srecv.at[n_dev + me], s2_s.at[o], s2_r.at[o], {"sp": to // n_dp, "dp": to % n_dp})

    row = lax.broadcasted_iota(jnp.int32, (span, span), 0)
    col = lax.broadcasted_iota(jnp.int32, (span, span), 1)
    lower = row >= col

    loads = [
        pltpu.make_async_copy(src, dst, in_s.at[n])
        for n, (src, dst) in enumerate(((v_hbm, v_ref), (u_hbm, u_ref), (d_hbm, d_ref)))
    ]
    for load in loads:
        load.start()
    barrier = pltpu.get_barrier_semaphore()

    def greet(o):
        to = (me + o) % n_dev
        pl.semaphore_signal(
            barrier, inc=1, device_id={"sp": to // n_dp, "dp": to % n_dp},
            device_id_type=pl.DeviceIdType.MESH,
        )
    each(1, n_dev, greet)
    pl.semaphore_wait(barrier, n_dev - 1)
    w_own().start()
    for k in range(1, pairs):
        w_x(k).start()
    wfull[dpi] = w_ref[...]

    def lanes(g):
        return pl.ds(pl.multiple_of(g * chans, chans), chans)

    def forward_group(g, half):
        wl = jnp.where(lower, wmix_ref[g], jnp.zeros((), BF16))
        bias = bias_ref[g]
        gain = gain_ref[g]
        shift = shift_ref[g]
        for b in range(nb):
            at = pl.ds(b * span, span)
            scaled, _ = norm_parts(gelu(v_ref[at, lanes(g)].astype(F32)))
            normed = (scaled * gain + shift).astype(BF16)
            mixed = mm(wl, normed, 1, 0) + bias
            out = (gelu(u_ref[at, lanes(g)].astype(F32)) * mixed).astype(BF16)
            got[pl.ds(pl.multiple_of(half * span, span), span), pl.ds(b * span, span)] = out.T

    def core_sum(k, q):
        t_core(k, q).wait_recv()
        g = gid(up(k), c, q)

        def one(j):
            a, b = j // n_z, j % n_z
            part[g, a, b] = (part[g, a, b].astype(F32) + rcore[k, q, a, b].astype(F32)).astype(BF16)
        each(0, n_sp, one)
        t_x(k, q).start()

    def forward_step(i):
        k = (i // gpc + 1) % pairs
        q = i % gpc
        keep = gid(up(k), c, q)
        give = gid(up(k), other, q)
        each(0, 2, lambda h: forward_group(gid(up(k), (c + h) % 2, q), h))

        def one(j):
            r = mm(got[...], d_ref[:, pl.ds(pl.multiple_of(j * width, width), width)], 1, 0)
            part[keep, j // n_z, j % n_z] = r[:span].astype(BF16)
            part[give, j // n_z, j % n_z] = r[span:].astype(BF16)
        each(0, n_sp, one)
        t_core(k, q).start()
        last = i - 1

        @pl.when((i > 0) & (last < (pairs - 1) * gpc))
        def _():
            core_sum((last // gpc + 1) % pairs, last % gpc)

    n_far = (pairs - 1) * gpc
    for load in loads:
        load.wait()
    each(0, n_far // 2, forward_step)
    for k in range(1, pairs):
        w_x(k).wait_recv()
        w_z(k).start()
        each(1, n_y, lambda o: w_y(k, 0, o).start())
    each(n_far // 2, n_far + 1, forward_step)
    for k in range(1, pairs):
        w_z(k).wait_recv()
        each(1, n_y, lambda o: w_y(k, 1, o).start())
    each(n_far + 1, n_far + gpc, forward_step)
    w_own().wait_recv()

    def forward_w():
        for k in range(1, pairs):
            each(1, n_y, lambda o: w_y(k, 0, o).wait_recv())
            each(1, n_y, lambda o: w_y(k, 1, o).wait_recv())
            w_fw(k).start()

    def yr_start(q):
        t_core(0, q).wait_recv()
        for k in range(1, pairs):
            t_x(k, q).wait_recv()
        g = gid(x, c, q)

        def one(j):
            a, b = j // n_z, j % n_z
            total = part[g, a, b].astype(F32) + rcore[0, q, a, b].astype(F32)
            for k in range(1, pairs):
                total = total + rx[k, q, a, b].astype(F32)
            part[g, a, b] = total.astype(BF16)
        each(0, n_sp, one)
        each(1, n_y, lambda o: t_yr(q, o).start())

    def zr_start(q):
        each(1, n_y, lambda o: t_yr(q, o).wait_recv())
        g = gid(x, c, q)

        def one(b):
            total = part[g, y, b].astype(F32)
            for o in range(1, n_y):
                total = total + ry[q, o, b].astype(F32)
            part[g, y, b] = total.astype(BF16)
        each(0, n_z, one)
        each(1, n_z, lambda o: t_zr(q, o).start())

    def za_start(q):
        each(1, n_z, lambda o: t_zr(q, o).wait_recv())
        total = part[gid(x, c, q), y, z].astype(F32)
        for o in range(1, n_z):
            total = total + rz[q, o].astype(F32)
        ag[q, y, z] = total.astype(BF16)
        each(1, n_z, lambda o: t_za(q, o).start())

    def ya_start(q):
        each(1, n_z, lambda o: t_za(q, o).wait_recv())
        each(1, n_y, lambda o: t_ya(q, o).start())

    sbuf[...] = jnp.zeros_like(sbuf)

    def backward_group(g, half):
        wl = jnp.where(lower, wmix_ref[g], jnp.zeros((), BF16))
        wlt = wl.T
        bias = bias_ref[g]
        gain = gain_ref[g]
        shift = shift_ref[g]
        acc[...] = jnp.zeros_like(acc)
        wl_ref[...] = wl
        wlt_ref[...] = wlt
        hl = pl.ds(pl.multiple_of(half * chans, chans), chans)
        for b in range(nb):
            at = pl.ds(b * span, span)
            gated, v_slope = gelu_both(v_ref[at, lanes(g)].astype(F32))
            scaled, inverse = norm_parts(gated)
            normed = (scaled * gain + shift).astype(BF16)
            mixed = mm(wl_ref[...], normed, 1, 0) + bias
            upper, u_slope = gelu_both(u_ref[at, lanes(g)].astype(F32))
            cot = gs[at, hl].astype(F32)
            dm = cot * upper
            dmb = dm.astype(BF16)
            gu_ref[at, lanes(g)] = (cot * mixed * u_slope).astype(BF16)
            acc[0] += dm
            acc[1] += mm(dmb, normed, 1, 1)
            dn = mm(wlt_ref[...], dmb, 1, 0)
            acc[2] += dn * scaled
            acc[3] += dn
            e = dn * gain
            m1 = jnp.mean(e, axis=-1, keepdims=True)
            m2 = jnp.mean(e * scaled, axis=-1, keepdims=True)
            gv_ref[at, lanes(g)] = (v_slope * (inverse * (e - m1 - scaled * m2))).astype(BF16)
        grad_w = jnp.where(lower, acc[1], 0.0)
        per = span // part_rows
        for p in range(per):
            sbuf[g * per + p, 0:part_rows, :] = grad_w[p * part_rows : (p + 1) * part_rows].astype(BF16)
        g_bias = jnp.sum(acc[0].T, axis=0, keepdims=True)
        g_gain = jnp.sum(acc[2], axis=0, keepdims=True)
        g_shift = jnp.sum(acc[3], axis=0, keepdims=True)
        r16 = lax.broadcasted_iota(jnp.int32, (16, chans), 0)
        extra = jnp.where(r16 == 0, g_bias, jnp.where(r16 == 1, g_gain, jnp.where(r16 == 2, g_shift, 0.0)))
        sbuf[g * per, part_rows : part_rows + 16, :] = extra.astype(BF16)
        for p in range(per):
            to = g * per + p

            @pl.when(to != me)
            def _(to=to):
                t_s1((to + n_dev - me) % n_dev).start()

    per_chunk = gpc // 2
    flat = wfull.reshape(n_dp, wfull.shape[1] * 2 * wfull.shape[3], wfull.shape[4])

    def stores(i):
        turn = i // per_chunk
        chunk = 2 * down(turn // 2) + (c + turn) % 2
        first = (chunk * gpc + 2 * (i % per_chunk)) * chans
        at = pl.ds(pl.multiple_of(first, 2 * chans), 2 * chans)
        return (
            pltpu.make_async_copy(gu_ref.at[:, at], gu_hbm.at[:, at], gu_s.at[i]),
            pltpu.make_async_copy(gv_ref.at[:, at], gv_hbm.at[:, at], gv_s.at[i]),
        )

    def backward_step(i):
        turn = i // per_chunk
        k = turn // 2
        chunk = 2 * down(k) + (c + turn) % 2
        two = i % per_chunk
        wrows = flat[chunk, pl.ds(pl.multiple_of(two * 2 * span, 2 * span), 2 * span), :]

        def one(j):
            at = pl.ds(pl.multiple_of(j * 2 * span, 2 * span), 2 * span)
            gs[at, :] = mm(d_ref[at, :], wrows, 1, 1).astype(BF16)
        each(0, rows // (2 * span), one)
        each(0, 2, lambda h: backward_group(chunk * gpc + 2 * two + h, h))
        for store in stores(i):
            store.start()

    n_steps = n_dp * per_chunk
    actions = {}

    def put(step, fn):
        actions.setdefault(min(step, n_steps - 1), []).append(fn)

    put(min(2, 2 * per_chunk - 2), forward_w)
    when = ((-1, 1, 3, 5), (0, 2, 4, 6), (2, 4, 6, 8), (4, 6, 8, 9))
    late = []
    stages = (yr_start, zr_start, za_start, ya_start)
    plan = [(when[q % 4][n], n, q) for q in range(gpc) for n in range(4)]
    for step, n, q in sorted(plan):
        fn = functools.partial(stages[n], q)
        if step < 0:
            fn()
        elif step < n_steps:
            put(step, fn)
        else:
            late.append(fn)

    def whole_step(i):
        turn = i // per_chunk
        for k in range(1, pairs):
            @pl.when(i == (2 * k + 1) * per_chunk)
            def _(k=k):
                w_fw(k).wait_recv()
        backward_step(i)
        for step in sorted(actions):
            @pl.when(i == step)
            def _(step=step):
                for fn in actions[step]:
                    fn()

    each(0, n_steps, whole_step)

    for fn in late[:2]:
        fn()
    each(1, n_dev, lambda o: t_s1(o).wait_recv())
    acc_s = sbuf[me].astype(F32)
    acc_s = lax.fori_loop(1, n_dev, lambda o, a: a + srecv[o].astype(F32), acc_s)
    each(1, n_dev, lambda o: t_s1(o).wait_send())
    sbuf[me] = acc_s.astype(BF16)
    srecv[n_dev + me] = acc_s.astype(BF16)
    each(1, n_dev, lambda o: t_s2(o).start())
    for fn in late[2:]:
        fn()

    for q in range(gpc):
        each(1, n_y, lambda o: t_ya(q, o).wait_recv())
        for j in range(n_sp):
            dw_ref[q * span : (q + 1) * span, j * width : (j + 1) * width] = ag[q, j // n_z, j % n_z]

    each(1, n_dev, lambda o: t_s2(o).wait_recv())
    sm_ref[...] = srecv[n_dev : 2 * n_dev]

    def stored(i):
        for store in stores(i):
            store.wait()
    each(0, n_steps, stored)

    w_own().wait_send()
    for k in range(1, pairs):
        w_x(k).wait_send()
        w_z(k).wait_send()
        each(1, n_y, lambda o: w_y(k, 0, o).wait_send())
        each(1, n_y, lambda o: w_y(k, 1, o).wait_send())
        w_fw(k).wait_send()
        each(0, gpc, lambda q: t_x(k, q).wait_send())
    for k in range(pairs):
        each(0, gpc, lambda q: t_core(k, q).wait_send())
    for q in range(gpc):
        each(1, n_y, lambda o: t_yr(q, o).wait_send())
        each(1, n_z, lambda o: t_zr(q, o).wait_send())
        each(1, n_z, lambda o: t_za(q, o).wait_send())
        each(1, n_y, lambda o: t_ya(q, o).wait_send())
    each(1, n_dev, lambda o: t_s2(o).wait_send())


def on_device(n_sp, n_dp, u_pre, v_pre, d_out, w_mix, mix_bias, norm_gain, norm_shift, w_out):
    _, rows, wide = u_pre.shape
    depth = d_out.shape[2]
    groups, span = w_mix.shape[:2]
    chans = wide // groups
    gpc = groups // n_dp
    width = depth // n_sp
    n_dev = n_sp * n_dp
    per = n_dev // groups
    part_rows = span // per
    shard = w_out.shape[0]
    pairs = n_dp // 2
    n_y = 1
    while 4 * n_y * n_y <= n_sp:
        n_y *= 2
    n_z = n_sp // n_y
    dims = (n_y, n_z, n_dp, gpc, span, chans, width, rows)
    dma = pltpu.SemaphoreType.DMA
    vm = pltpu.VMEM
    piece = (n_y, n_z, span, width)
    w_piece = (n_y, 2, shard // (2 * n_y), depth)
    n_steps = groups // 2
    scratch = [
        vm((rows, wide), BF16), vm((rows, wide), BF16), vm((rows, depth), BF16),
        vm((rows, wide), BF16), vm((rows, wide), BF16),
        dma((3,)), dma((n_steps,)), dma((n_steps,)),
        vm((n_dp,) + w_piece, BF16),
        vm((groups,) + piece, BF16),
        vm((pairs, gpc) + piece, BF16),
        vm((pairs, gpc) + piece, BF16),
        vm((gpc,) + piece, BF16),
        vm((gpc,) + piece[1:2] + piece[2:], BF16),
        vm((gpc,) + piece, BF16),
        vm((rows, 2 * chans), BF16),
        vm((2 * chans, rows), BF16),
        vm((span, span), BF16),
        vm((span, span), BF16),
        vm((4, span, chans), F32),
        vm((n_dev, part_rows + 16, chans), BF16),
        vm((2 * n_dev, part_rows + 16, chans), BF16),
        dma, dma,
        dma((pairs,)), dma((pairs,)),
        dma((pairs,)), dma((pairs,)),
        dma((pairs, 2, n_y)), dma((pairs, 2, n_y)),
        dma((pairs,)), dma((pairs,)),
        dma((pairs, gpc)), dma((pairs, gpc)),
        dma((pairs, gpc)), dma((pairs, gpc)),
        dma((gpc, n_y)), dma((gpc, n_y)),
        dma((gpc, n_z)), dma((gpc, n_z)),
        dma((gpc, n_z)), dma((gpc, n_z)),
        dma((gpc, n_y)), dma((gpc, n_y)),
        dma((n_dev,)), dma((n_dev,)),
        dma((n_dev,)), dma((n_dev,)),
    ]
    spec = pl.BlockSpec(memory_space=pltpu.VMEM)
    hbm = pl.BlockSpec(memory_space=pl.ANY)
    gu, gv, dw, sm = pl.pallas_call(
        functools.partial(kernel, dims),
        out_shape=(
            jax.ShapeDtypeStruct((rows, wide), BF16),
            jax.ShapeDtypeStruct((rows, wide), BF16),
            jax.ShapeDtypeStruct((shard, depth), BF16),
            jax.ShapeDtypeStruct((n_dev, part_rows + 16, chans), BF16),
        ),
        in_specs=[hbm] * 3 + [spec] * 5,
        out_specs=(hbm, hbm, spec, spec),
        scratch_shapes=scratch,
        compiler_params=pltpu.CompilerParams(collective_id=0, has_side_effects=True, vmem_limit_bytes=67043328),
    )(
        u_pre[0], v_pre[0], d_out[0], w_mix,
        jnp.broadcast_to(mix_bias[:, :, None], (groups, span, chans)),
        norm_gain[:, None, :], norm_shift[:, None, :],
        w_out.reshape(w_piece),
    )
    grad_w = sm[:, :part_rows].reshape(groups, span, span).astype(F32)
    extra = sm.reshape(groups, per, part_rows + 16, chans)[:, 0, part_rows:].astype(F32)
    return (gu[None], gv[None], dw.astype(F32), grad_w, extra[:, 0], extra[:, 1], extra[:, 2])


def solution(mesh):
    body = functools.partial(on_device, mesh.shape["sp"], mesh.shape["dp"])
    return jax.shard_map(
        body,
        mesh=mesh,
        in_specs=(
            P("dp", "sp", None),
            P("dp", "sp", None),
            P("dp", "sp", None),
            P(),
            P(),
            P(),
            P(),
            P("dp", None),
        ),
        out_specs=(P("dp", "sp", None), P("dp", "sp", None), P("dp", None), P(), P(), P(), P()),
        check_vma=False,
    )
```
